32 devices in a mesh: ep: 8 (over z, y), tp: 4 (over x, core).
Axes of the slice: x: 2, y: 2, z: 4, core: 2. Of those that a mesh axis runs over, the one named last changes fastest.
Arguments:
- queries: bfloat16 [1536, 2048], P('ep', 'tp'), may hold values from -8 to 8
- keys: bfloat16 [1536, 512], P('ep', 'tp'), may hold values from -8 to 8
- values: bfloat16 [1536, 512], P('ep', 'tp'), may hold values from -6 to 6
- query_gain: float32 [2048], P('tp'), may hold values from 0.5 to 6
- key_gain: float32 [512], P('tp'), may hold values from 0.7 to 6
- out_weight: bfloat16 [2048, 4096], P('tp'), may hold values from -0.125 to 0.125
- expert_input: bfloat16 [2048, 4096], P(('ep', 'tp')), may hold values from -6 to 6
- norm_gain: float32 [4096], replicated, may hold values from 0.1 to 1.9
- routes: int32 [2048, 2], P(('ep', 'tp')), may hold values from 0 to 7, all different within a row; in each aligned block of 64 rows (0 to 63, 64 to 127, ...) at most 32 rows name the same one
- route_weight: float32 [2048, 2], P(('ep', 'tp')), may hold values from 0.2 to 2
- gate_weight: bfloat16 [8, 4096, 1024], P('ep', None, 'tp'), may hold values from -0.09375 to 0.09375
- up_weight: bfloat16 [8, 4096, 1024], P('ep', None, 'tp'), may hold values from -0.09375 to 0.09375
- down_weight: bfloat16 [8, 1024, 4096], P('ep', 'tp'), may hold values from -0.1875 to 0.1875
Outputs:
- mixed: bfloat16 [1536, 4096], P(('ep', 'tp'))
- moe_out: bfloat16 [2048, 4096], P(('ep', 'tp'))
The draws below stay inside these ranges and needn't reach their ends.
Inputs may be any that keep to these rules, and one draw needn't show every extreme that they name: `routes`: each row names 2 different experts; in the rows of one device no expert is named by more than 32 rows, and in some device one expert is named by exactly 32 rows.
All inputs are finite; a program needn't handle non-finite values.
Results may differ from the reference program's by a relative error of at most 0.013.
The reference program's roundings to bfloat16 on the way count: a program that leaves them out, or rounds other values in their place, can miss the bound.
Values may be sent and summed in bfloat16 or wider, within the bound.
A program may use at most 128 MiB of HBM per device.

```python
import math
import jax
import jax.numpy as jnp
import numpy as np
from jax import lax

D = 4096
HEADS = 32
KV_HEADS = 8
HEAD_DIM = 64
EXPERT_WIDTH = 1024
TOP = 2
GRID_W = 128
TOK_EXP = 64
TOKENS = 1536
EXP_TOKENS = 2048
EXPERTS = 8
CAP = 32
N_EP = 8
N_TP = 4


def attention_fields(key):
    base = jax.random.fold_in(key, 911)
    subkeys = jax.random.split(base, 6)
    query_level = jnp.exp(jax.random.uniform(subkeys[0], (HEADS,), jnp.float32, 0.0, math.log(2.2)))
    key_level = jnp.exp(jax.random.uniform(subkeys[1], (KV_HEADS,), jnp.float32, 0.0, math.log(2.2)))
    query_gain = jnp.repeat(query_level, HEAD_DIM) * jax.random.uniform(subkeys[2], (HEADS * HEAD_DIM,), jnp.float32, 0.7, 1.3)
    key_gain = jnp.repeat(key_level, HEAD_DIM) * jax.random.uniform(subkeys[3], (KV_HEADS * HEAD_DIM,), jnp.float32, 0.7, 1.3)
    queries = jnp.clip(jax.random.normal(subkeys[4], (TOKENS, HEADS * HEAD_DIM), jnp.float32), -6.0, 6.0)
    keys = jnp.clip(jax.random.normal(subkeys[5], (TOKENS, KV_HEADS * HEAD_DIM), jnp.float32), -6.0, 6.0)
    return (queries, keys, query_gain, key_gain)


def draw_queries(key, part):
    return attention_fields(key)[0].astype(jnp.bfloat16)


def draw_keys(key, part):
    return attention_fields(key)[1].astype(jnp.bfloat16)


def draw_query_gain(key, part):
    return attention_fields(key)[2].astype(jnp.float32)


def draw_key_gain(key, part):
    return attention_fields(key)[3].astype(jnp.float32)


def shard_levels(key, shape, shards, least, largest):
    def one(position, shards_of):
        steps = jax.random.uniform(jax.random.fold_in(jax.random.fold_in(key, 6), position), (shards_of,), jnp.float32, least / len(shards), largest / len(shards))
        return jnp.repeat(jnp.exp(steps), shape[position] // shards_of).reshape((-1,) + (1,) * (len(shape) - position - 1))

    level = one(*shards[0])
    for cut in shards[1:]:
        level = level * one(*cut)
    return level


def routed_block(rng, own, number, rows, number_of, top, reach, lean):
    ranking = jax.random.permutation(rng, number_of)
    heavy_load, common = portions_of(number_of, rows * top, reach, lean, True), portions_of(number_of, rows * top, reach, lean, False)
    places = jnp.arange(number_of)

    def named(lengths, turn):
        used = int((lengths > 0).sum())
        fixed = max(1, used // 4)
        shifted = fixed + (places - fixed + turn * (used - fixed)) % max(1, number_of - fixed)
        return jnp.zeros((number_of,), jnp.int32).at[ranking[jnp.where(places < fixed, places, shifted)]].set(jnp.asarray(lengths, jnp.int32))

    lengths = jnp.where(number % 4 == 0, named(heavy_load, number // 4), named(common, number - number // 4 - 1))
    mixed = jax.random.permutation(jax.random.fold_in(own, 3), number_of)
    source_of, receiver = mixed[0:number_of // 2 * 2:2], mixed[1:number_of // 2 * 2:2]
    slack = jnp.minimum(lengths[source_of] - 1, reach - lengths[receiver]) // 2
    slack = jnp.where((source_of == ranking[0]) | (receiver == ranking[0]) | (lengths[receiver] == 0), 0, jnp.maximum(slack, 0))
    shifted = jax.random.randint(jax.random.fold_in(own, 4), (number_of // 2,), 0, 1 << 20) % (slack + 1)
    lengths = lengths.at[source_of].add(-shifted).at[receiver].add(shifted)
    labels = jnp.searchsorted(jnp.cumsum(lengths), jnp.arange(rows * top), side="right").astype(jnp.int32)
    grid = labels.reshape(top, rows).T
    grid = grid[jax.random.permutation(jax.random.fold_in(own, 1), rows)]
    turn = jax.random.randint(jax.random.fold_in(own, 2), (rows, 1), 0, top)
    return jnp.take_along_axis(grid, (jnp.arange(top)[None, :] + turn) % top, axis=1)


def portions_of(number_of, total, reach, slope, full):
    weights = [(1 << 20) // math.isqrt(standing ** slope) + 1 for standing in range(1, number_of + 1)]
    largest = reach if full else min(reach, max(-(-total // number_of), total * weights[0] // sum(weights)))
    least = 1 if total - largest >= number_of - 1 else 0
    given, rest = [largest] + [least] * (number_of - 1), total - largest - least * (number_of - 1)
    while rest > 0:
        movable = [i for i in range(1, number_of) if given[i] < largest] or [i for i in range(1, number_of) if given[i] < reach]
        mass, budget = sum([weights[i] for i in movable]), rest
        for i in movable:
            extra = min(reach - given[i], max(1, budget * weights[i] // mass), rest)
            given[i] = given[i] + extra
            rest = rest - extra
    return np.array(given)


def normal_values(rng, extent, scale, reach, shards=(), kind=jnp.bfloat16):
    values = scale * jax.random.normal(rng, extent, jnp.float32)
    if shards:
        values = values * shard_levels(rng, extent, shards, -0.22, 0.18)
    return jnp.clip(values, -reach, reach).astype(kind)


def setup_inputs(seed: int = 0) -> dict:
    arg_keys = jax.random.split(jax.random.key(seed), 14)
    queries = draw_queries(jax.random.fold_in(arg_keys[13], 71), 0)
    keys = draw_keys(jax.random.fold_in(arg_keys[13], 71), 0)
    values = normal_values(arg_keys[2], (TOKENS, KV_HEADS * HEAD_DIM), 1.0, 6.0, ((0, 8), (1, 4)))
    query_gain = draw_query_gain(jax.random.fold_in(arg_keys[13], 71), 0)
    key_gain = draw_key_gain(jax.random.fold_in(arg_keys[13], 71), 0)
    out_weight = normal_values(arg_keys[5], (HEADS * HEAD_DIM, D), (HEADS * HEAD_DIM) ** -0.5, 0.125, ((0, 4),))
    expert_input = normal_values(arg_keys[6], (EXP_TOKENS, D), 1.0, 6.0, ((0, 32),))
    norm_gain = jnp.clip(1.0 + 0.18 * jax.random.normal(arg_keys[7], (D,), jnp.float32), 0.1, 1.9)
    routes_keys = jax.random.split(jax.random.fold_in(arg_keys[8], 1), EXP_TOKENS // TOK_EXP)
    routes_turns = jax.random.permutation(jax.random.fold_in(arg_keys[8], 3), EXP_TOKENS // TOK_EXP)
    routes = jax.vmap(lambda own, number: routed_block(jax.random.fold_in(arg_keys[8], 2), own, number, TOK_EXP, EXPERTS, TOP, CAP, 2))(routes_keys, routes_turns).reshape((EXP_TOKENS, TOP))
    route_weight = jnp.clip(jnp.exp(math.log(2.0) - 2.3025851 * jax.random.uniform(arg_keys[9], (EXP_TOKENS, TOP), jnp.float32) ** shard_levels(arg_keys[9], (EXP_TOKENS, TOP), ((0, 32),), -0.2, 0.2)), 0.2, 2.0)
    gate_weight = normal_values(arg_keys[10], (EXPERTS, D, EXPERT_WIDTH), D ** -0.5, 0.09375, ((0, 8), (2, 4)))
    up_weight = normal_values(arg_keys[11], (EXPERTS, D, EXPERT_WIDTH), D ** -0.5, 0.09375, ((0, 8), (2, 4)))
    down_weight = normal_values(arg_keys[12], (EXPERTS, EXPERT_WIDTH, D), EXPERT_WIDTH ** -0.5, 0.1875, ((0, 8), (1, 4)))
    return {"queries": queries, "keys": keys, "values": values, "query_gain": query_gain, "key_gain": key_gain, "out_weight": out_weight, "expert_input": expert_input, "norm_gain": norm_gain, "routes": routes, "route_weight": route_weight, "gate_weight": gate_weight, "up_weight": up_weight, "down_weight": down_weight}


NORM_EPS = 1e-06
ROPE_BASE = 10000.0

def round_trip(matrix):
    return lax.optimization_barrier(matrix.astype(jnp.bfloat16)).astype(jnp.float32)

def rotate(vectors, grid_rows, grid_cols):
    quarter = vectors.shape[-1] // 4
    inverse = ROPE_BASE ** (-jnp.arange(quarter, dtype=jnp.float32) / quarter)
    angle_row = grid_rows[:, None] * inverse
    angle_col = grid_cols[:, None] * inverse
    angles = jnp.concatenate([angle_row, angle_row, angle_col, angle_col], axis=-1)[:, None, :]
    part_one, part_two, part_three, part_four = jnp.split(vectors, 4, axis=-1)
    turned = jnp.concatenate([-part_two, part_one, -part_four, part_three], axis=-1)
    return vectors * jnp.cos(angles) + turned * jnp.sin(angles)

def head_norm(raw_rows, gains, head_count, offset):
    row_count = raw_rows.shape[0]
    flat_rows = raw_rows.astype(jnp.float32).reshape(row_count, head_count, -1)
    unit_vec = flat_rows * lax.rsqrt(lax.optimization_barrier(jnp.mean(flat_rows * flat_rows, axis=-1, keepdims=True)) + NORM_EPS)
    unit_vec = unit_vec * gains.reshape(head_count, -1)
    places = offset + jnp.arange(row_count, dtype=jnp.int32)
    grid_rows = (places // GRID_W).astype(jnp.float32)
    grid_cols = (places % GRID_W).astype(jnp.float32)
    return rotate(unit_vec, grid_rows, grid_cols).astype(jnp.bfloat16)

def attend_block(query_block, key_head, value_head, score_scale):
    scores = jnp.einsum('qgd,kd->gqk', query_block.astype(jnp.float32), key_head.astype(jnp.float32)) * score_scale
    row_max = lax.optimization_barrier(jnp.max(scores, axis=-1, keepdims=True))
    weights = jnp.exp(scores - row_max)
    weight_sum = lax.optimization_barrier(jnp.sum(weights, axis=-1))
    rounded = round_trip(weights)
    summed = jnp.einsum('gqk,kd->qgd', rounded, value_head.astype(jnp.float32))
    return (summed / jnp.transpose(weight_sum)[:, :, None]).astype(jnp.bfloat16)

def attention(q_turned, k_turned, values):
    tokens = q_turned.shape[0]
    group_size = HEADS // KV_HEADS
    query_span = math.gcd(tokens, 256)
    score_scale = HEAD_DIM ** (-0.5)
    query_heads = q_turned.reshape(tokens // query_span, query_span, KV_HEADS, group_size, HEAD_DIM)
    query_heads = jnp.transpose(query_heads, (2, 0, 1, 3, 4))
    key_heads = jnp.transpose(k_turned.reshape(tokens, KV_HEADS, HEAD_DIM), (1, 0, 2))
    value_heads = jnp.transpose(values.reshape(tokens, KV_HEADS, HEAD_DIM), (1, 0, 2))

    def per_head(operands):
        query_blocks, key_head, value_head = operands

        def per_block(query_block):
            return attend_block(query_block, key_head, value_head, score_scale)
        return lax.map(per_block, query_blocks)
    attended = lax.map(per_head, (query_heads, key_heads, value_heads))
    return jnp.transpose(attended, (1, 2, 0, 3, 4)).reshape(tokens, HEADS * HEAD_DIM)

def routed_experts(expert_input, norm_gain, routes, route_weight, gate_weight, up_weight, down_weight):
    row_count = expert_input.shape[0]
    as_float = expert_input.astype(jnp.float32)
    normed = (as_float * lax.rsqrt(lax.optimization_barrier(jnp.mean(as_float * as_float, axis=-1, keepdims=True)) + NORM_EPS) * norm_gain).astype(jnp.bfloat16)
    flat_routes = routes.reshape(-1).astype(jnp.int32)
    flat_weight = route_weight.reshape(-1)
    sorted_ids = jnp.argsort(flat_routes, stable=True).astype(jnp.int32)
    counts = lax.optimization_barrier(jnp.sum((flat_routes[:, None] == jnp.arange(EXPERTS, dtype=jnp.int32)[None, :]).astype(jnp.int32), axis=0)).astype(jnp.int32)
    starts = (jnp.cumsum(counts) - counts).astype(jnp.int32)
    most_rows = N_EP * N_TP * CAP
    padded = jnp.concatenate([sorted_ids, jnp.zeros((most_rows,), jnp.int32)])
    part_width = EXPERT_WIDTH // N_TP

    def one_expert(combined, expert_id):
        picked = lax.dynamic_slice(padded, (starts[expert_id],), (most_rows,))
        is_live = jnp.arange(most_rows, dtype=jnp.int32) < counts[expert_id]
        token_ids = (picked // TOP).astype(jnp.int32)
        gathered = normed[token_ids]
        gate_out = jnp.dot(gathered, gate_weight[expert_id], preferred_element_type=jnp.float32)
        up_out = jnp.dot(gathered, up_weight[expert_id], preferred_element_type=jnp.float32)
        hidden = (jax.nn.silu(gate_out) * up_out).astype(jnp.bfloat16)
        down_one = down_weight[expert_id]
        result = jnp.zeros((most_rows, D), jnp.float32)
        for part_id in range(N_TP):
            partial_value = jnp.dot(hidden[:, part_id * part_width:(part_id + 1) * part_width], down_one[part_id * part_width:(part_id + 1) * part_width], preferred_element_type=jnp.float32)
            result = result + round_trip(partial_value)
        result = round_trip(result)
        scaled = jnp.where(is_live[:, None], result * flat_weight[picked][:, None], 0.0)
        return (combined.at[token_ids].add(scaled), None)
    combined, unused = lax.scan(one_expert, jnp.zeros((row_count, D), jnp.float32), jnp.arange(EXPERTS, dtype=jnp.int32))
    return combined.astype(jnp.bfloat16)

def reference(queries, keys, values, query_gain, key_gain, out_weight, expert_input, norm_gain, routes, route_weight, gate_weight, up_weight, down_weight):
    q_turned = head_norm(queries, query_gain, HEADS, 0)
    k_turned = head_norm(keys, key_gain, KV_HEADS, 0)
    attended = attention(q_turned, k_turned, values)
    tokens = attended.shape[0]
    part_width = HEADS * HEAD_DIM // N_TP
    mixed_sum = jnp.zeros((tokens, D), jnp.float32)
    for part_id in range(N_TP):
        partial_value = jnp.dot(attended[:, part_id * part_width:(part_id + 1) * part_width], out_weight[part_id * part_width:(part_id + 1) * part_width], preferred_element_type=jnp.float32)
        mixed_sum = mixed_sum + round_trip(partial_value)
    mixed = mixed_sum.astype(jnp.bfloat16)
    moe_out = routed_experts(expert_input, norm_gain, routes, route_weight, gate_weight, up_weight, down_weight)
    return (mixed, moe_out)
```

```python
import functools

import jax
import jax.numpy as jnp
from jax import lax
from jax.experimental import pallas as pl
from jax.experimental.pallas import tpu as pltpu
from jax.sharding import PartitionSpec as P

HEAD_DIM = 64
GRID_W = 128


NORM_EPS = 1e-06
ROPE_BASE = 10000.0


def rotate(vectors, grid_rows, grid_cols):
    quarter = vectors.shape[-1] // 4
    inverse = ROPE_BASE ** (-jnp.arange(quarter, dtype=jnp.float32) / quarter)
    angle_row = grid_rows[:, None] * inverse
    angle_col = grid_cols[:, None] * inverse
    angles = jnp.concatenate([angle_row, angle_row, angle_col, angle_col], axis=-1)[:, None, :]
    part_one, part_two, part_three, part_four = jnp.split(vectors, 4, axis=-1)
    turned = jnp.concatenate([-part_two, part_one, -part_four, part_three], axis=-1)
    return vectors * jnp.cos(angles) + turned * jnp.sin(angles)


def head_norm(raw_rows, gains, head_count, offset):
    row_count = raw_rows.shape[0]
    flat_rows = raw_rows.astype(jnp.float32).reshape(row_count, head_count, -1)
    unit_vec = flat_rows * lax.rsqrt(
        jnp.mean(flat_rows * flat_rows, axis=-1, keepdims=True) + NORM_EPS
    )
    unit_vec = unit_vec * gains.reshape(head_count, -1)
    places = offset + jnp.arange(row_count, dtype=jnp.int32)
    grid_rows = (places // GRID_W).astype(jnp.float32)
    grid_cols = (places % GRID_W).astype(jnp.float32)
    return rotate(unit_vec, grid_rows, grid_cols).astype(jnp.bfloat16).reshape(row_count, -1)


def absorb(running, key_block, value_block, grouped, score_scale):
    run_max, weight_sum, summed = running
    kv_count = grouped.shape[1]
    key_heads = key_block.reshape(key_block.shape[0], kv_count, -1)
    value_heads = value_block.reshape(value_block.shape[0], kv_count, -1)
    scores = (
        jnp.einsum("qhgd,khd->hgqk", grouped, key_heads, preferred_element_type=jnp.float32)
        * score_scale
    )
    new_max = jnp.maximum(run_max, jnp.max(scores, axis=-1))
    rescale = jnp.exp(run_max - new_max)
    weights = jnp.exp(scores - new_max[..., None])
    weight_sum = weight_sum * rescale + jnp.sum(weights, axis=-1)
    update = jnp.einsum(
        "hgqk,khd->qhgd",
        weights.astype(jnp.bfloat16),
        value_heads,
        preferred_element_type=jnp.float32,
    )
    summed = summed * jnp.transpose(rescale, (2, 0, 1))[..., None] + update
    return (new_max, weight_sum, summed)


def run_experts(sending, gate_weight, up_weight, down_weight):
    arrived = lax.all_to_all(sending, "ep", split_axis=0, concat_axis=0, tiled=True)
    shard_rows = lax.all_gather(arrived, "tp", axis=0, tiled=True)
    gate_out = jnp.dot(shard_rows, gate_weight[0], preferred_element_type=jnp.float32)
    up_out = jnp.dot(shard_rows, up_weight[0], preferred_element_type=jnp.float32)
    hidden = (jax.nn.silu(gate_out) * up_out).astype(jnp.bfloat16)
    results = lax.psum_scatter(
        jnp.dot(hidden, down_weight[0], preferred_element_type=jnp.float32).astype(jnp.bfloat16),
        "tp",
        scatter_dimension=0,
        tiled=True,
    )
    return lax.all_to_all(results, "ep", split_axis=0, concat_axis=0, tiled=True)


MESH = pl.DeviceIdType.MESH
TILE = 1024


def flip(index, pattern, size):
    result = 0
    bit = 1
    while bit < size:
        both = lax.rem(lax.div(index, bit) + lax.div(pattern, bit), 2)
        result = result + both * bit
        bit = bit * 2
    return result


def fused_kernel(
    n,
    laid,
    q_ref,
    kv_ref,
    wg_hbm,
    wu_hbm,
    wd_hbm,
    ow_hbm,
    back,
    mixed,
    wg,
    wu,
    wd,
    ow,
    rows,
    partial,
    red,
    q_send,
    x_got,
    y_send,
    kv_all,
    attended,
    m_part,
    m_red,
    m_send,
    m_got,
    load_sem,
    kv_sems,
    disp_sems,
    fwd_sems,
    red_sems,
    ret_sems,
    mix_sems,
):
    e = lax.axis_index("ep")
    t = lax.axis_index("tp")
    side = lax.div(t, 2)
    core = lax.rem(t, 2)
    other_side = 1 - side
    other_core = 1 - core
    x_peer = (e, other_side * 2 + core)
    c_peer = (e, side * 2 + other_core)
    cap, width = laid.shape[1], laid.shape[2]
    pairs = attended.shape[0]
    tok = attended.shape[1]

    def remote(src, dst, send, recv, device):
        return pltpu.make_async_remote_copy(
            src_ref=src, dst_ref=dst, send_sem=send, recv_sem=recv, device_id=device, device_id_type=MESH
        )

    loads = [
        pltpu.make_async_copy(a, b, load_sem.at[k])
        for k, (a, b) in enumerate([(ow_hbm, ow), (wg_hbm, wg), (wu_hbm, wu), (wd_hbm, wd)])
    ]
    for load in loads:
        load.start()

    barrier = pltpu.get_barrier_semaphore()
    for s in range(1, n):
        pl.semaphore_signal(barrier, inc=1, device_id=(flip(e, s, n), t), device_id_type=MESH)
    pl.semaphore_signal(barrier, inc=1, device_id=x_peer, device_id_type=MESH)
    pl.semaphore_signal(barrier, inc=1, device_id=c_peer, device_id_type=MESH)
    pl.semaphore_wait(barrier, n + 1)

    def kv_direct(s):
        return remote(kv_ref, kv_all.at[:, e], kv_sems.at[0, s], kv_sems.at[1, s], (flip(e, s, n), t))

    def kv_direct_in(s):
        return remote(kv_ref, kv_all.at[:, flip(e, s, n)], kv_sems.at[0, s], kv_sems.at[1, s], (flip(e, s, n), t))

    def kv_relay(s):
        owner = flip(e, s, n)
        return remote(kv_all.at[:, owner], kv_all.at[:, owner], kv_sems.at[0, s + 1], kv_sems.at[1, s + 1], (flip(e, 1, n), t))

    def kv_relay_in(s):
        owner = flip(e, s + 1, n)
        return remote(kv_all.at[:, owner], kv_all.at[:, owner], kv_sems.at[0, s + 1], kv_sems.at[1, s + 1], (flip(e, 1, n), t))

    def pattern(i):
        return jnp.where(i < n // 2, 2 * i, 2 * (n - 1 - i) + 1)

    def dispatch(i):
        s = pattern(i)
        return remote(laid.at[flip(e, s, n)], rows.at[e, t], disp_sems.at[0, i], disp_sems.at[1, i], (flip(e, s, n), t))

    def dispatch_in(i):
        s = pattern(i)
        return remote(laid.at[flip(e, s, n)], rows.at[flip(e, s, n), t], disp_sems.at[0, i], disp_sems.at[1, i], (flip(e, s, n), t))

    def owner_of(i):
        return flip(e, pattern(i), n)

    def to_side(i):
        o = owner_of(i)
        return remote(rows.at[o, t], rows.at[o, t], fwd_sems.at[0, 0, i], fwd_sems.at[1, 0, i], x_peer)

    def from_side(i):
        o = owner_of(i)
        return remote(rows.at[o, t], rows.at[o, other_side * 2 + core], fwd_sems.at[0, 0, i], fwd_sems.at[1, 0, i], x_peer)

    def to_core(i):
        o = owner_of(i)
        return remote(rows.at[o, t], rows.at[o, t], fwd_sems.at[0, 1, i], fwd_sems.at[1, 1, i], c_peer)

    def from_core(i):
        o = owner_of(i)
        return remote(rows.at[o, t], rows.at[o, side * 2 + other_core], fwd_sems.at[0, 1, i], fwd_sems.at[1, 1, i], c_peer)

    def relay_core(i):
        o = owner_of(i)
        slot = other_side * 2 + core
        return remote(rows.at[o, slot], rows.at[o, slot], fwd_sems.at[0, 2, i], fwd_sems.at[1, 2, i], c_peer)

    def relayed_core(i):
        o = owner_of(i)
        slot = other_side * 2 + core
        return remote(rows.at[o, slot], rows.at[o, other_side * 2 + other_core], fwd_sems.at[0, 2, i], fwd_sems.at[1, 2, i], c_peer)

    def reduce_core(i):
        return remote(partial.at[i, :, other_core], red.at[i], red_sems.at[0, 0, i], red_sems.at[1, 0, i], c_peer)

    def reduce_side(i):
        return remote(q_send.at[i], x_got.at[i], red_sems.at[0, 1, i], red_sems.at[1, 1, i], x_peer)

    def give_back(i):
        o = owner_of(i)
        return remote(y_send.at[i], back.at[e], ret_sems.at[0, i], ret_sems.at[1, i], (o, t))

    def get_back(i):
        o = owner_of(i)
        return remote(y_send.at[i], back.at[o], ret_sems.at[0, i], ret_sems.at[1, i], (o, t))

    mix_core = remote(m_part.at[:, other_core], m_red, mix_sems.at[0, 0], mix_sems.at[1, 0], c_peer)
    mix_side = remote(m_send, m_got, mix_sems.at[0, 1], mix_sems.at[1, 1], x_peer)

    own = pltpu.make_async_copy(laid.at[e], rows.at[e, t], load_sem.at[4])
    own_kv = pltpu.make_async_copy(kv_ref, kv_all.at[:, e], load_sem.at[5])
    own.start()
    own_kv.start()
    for s in range(2, n, 2):
        kv_direct(s).start()
    kv_direct(1).start()
    for i in range(1, n):
        dispatch(i).start()
    own.wait()
    to_side(0).start()
    to_core(0).start()
    own_kv.wait()

    def attend(pair):
        kv = kv_all[lax.div(pair * 2 * kv_all.shape[0], pairs * 2)].reshape(n * tok, 128)
        halves = []
        for h in range(2):
            scores = lax.dot_general(
                q_ref[pair * 2 + h], kv, (((1,), (1,)), ((), ())), preferred_element_type=jnp.float32
            ) * (HEAD_DIM ** (-0.5))
            peak = jnp.max(scores, axis=1, keepdims=True)
            weights = jnp.exp(scores - peak)
            total = jnp.sum(weights, axis=1, keepdims=True)
            summed = jnp.dot(weights.astype(jnp.bfloat16), kv, preferred_element_type=jnp.float32)
            halves.append(summed / total)
        lane = lax.broadcasted_iota(jnp.int32, halves[0].shape, 1)
        joined = jnp.where(lane < HEAD_DIM, pltpu.roll(halves[0], HEAD_DIM, 1), halves[1])
        attended[pair] = joined.astype(jnp.bfloat16)

    def f32(value):
        return value.astype(jnp.float32)

    def step(i, carry):
        @pl.when(jnp.logical_and(i > 0, i < n))
        def _():
            dispatch_in(i).wait_recv()
            to_side(i).start()
            to_core(i).start()

        @pl.when(i == 0)
        def _():
            for s in range(2, n, 2):
                kv_direct_in(s).wait_recv()
                kv_relay(s).start()

        @pl.when(i == 1)
        def _():
            kv_direct_in(1).wait_recv()
            for s in range(2, n, 2):
                kv_relay_in(s).wait_recv()

        @pl.when(jnp.logical_and(i >= 1, i <= n))
        def _():
            from_side(i - 1).wait_recv()
            relay_core(i - 1).start()

        @pl.when(jnp.logical_and(i >= 1, i <= pairs))
        def _():
            attend(i - 1)

        @pl.when(i == pairs + 1)
        def _():
            loads[0].wait()
            for tile in range(0, width, TILE):
                product = jnp.dot(attended[0], ow[0, :, tile:tile + TILE], preferred_element_type=jnp.float32)
                for p in range(1, pairs):
                    product += jnp.dot(attended[p], ow[p, :, tile:tile + TILE], preferred_element_type=jnp.float32)
                m_part[:, :, :, tile:tile + TILE] = product.astype(jnp.bfloat16).reshape(2, 2, tok // 4, TILE)
            mix_core.start()

        @pl.when(i == pairs + 2)
        def _():
            mix_core.wait_recv()
            m_send[...] = (f32(m_part[other_side, core]) + f32(m_red[other_side])).astype(jnp.bfloat16)
            mix_side.start()

        @pl.when(jnp.logical_and(i >= 2, i < n + 2))
        def _():
            k = i - 2

            @pl.when(k == 0)
            def _():
                for load in loads[1:]:
                    load.wait()

            from_core(k).wait_recv()
            relayed_core(k).wait_recv()
            tokens = rows[owner_of(k)].reshape(4 * cap, width)
            gate = jnp.dot(tokens, wg[...], preferred_element_type=jnp.float32)
            up = jnp.dot(tokens, wu[...], preferred_element_type=jnp.float32)
            hidden = (gate / (1.0 + jnp.exp(-gate)) * up).astype(jnp.bfloat16)
            for tile in range(0, width, TILE):
                product = jnp.dot(hidden, wd[:, tile:tile + TILE], preferred_element_type=jnp.float32)
                partial[k, :, :, :, tile:tile + TILE] = product.astype(jnp.bfloat16).reshape(2, 2, cap, TILE)
            reduce_core(k).start()

        @pl.when(jnp.logical_and(i >= 3, i < n + 3))
        def _():
            k = i - 3
            reduce_core(k).wait_recv()
            q_send[k] = (f32(partial[k, other_side, core]) + f32(red[k, other_side])).astype(jnp.bfloat16)
            reduce_side(k).start()

        @pl.when(jnp.logical_and(i >= 4, i < n + 4))
        def _():
            k = i - 4
            reduce_side(k).wait_recv()
            y = (f32(partial[k, side, core]) + f32(red[k, side]) + f32(x_got[k])).astype(jnp.bfloat16)

            @pl.when(k == 0)
            def _():
                back[e] = y

            @pl.when(k > 0)
            def _():
                y_send[k] = y
                give_back(k).start()

        return carry

    lax.fori_loop(0, n + 4, step, 0)

    mix_side.wait_recv()
    mixed[...] = (f32(m_part[side, core]) + f32(m_red[side]) + f32(m_got[...])).astype(jnp.bfloat16)
    mix_core.wait_send()
    mix_side.wait_send()
    for s in range(2, n, 2):
        kv_direct(s).wait_send()
        kv_relay(s).wait_send()
    kv_direct(1).wait_send()

    def drain(i, carry):
        @pl.when(i > 0)
        def _():
            dispatch(i).wait_send()
            give_back(i).wait_send()
            get_back(i).wait_recv()

        to_side(i).wait_send()
        to_core(i).wait_send()
        relay_core(i).wait_send()
        reduce_core(i).wait_send()
        reduce_side(i).wait_send()
        return carry

    lax.fori_loop(0, n, drain, 0)


def fused(laid, q_heads, kv_pack, gate_weight, up_weight, down_weight, out_weight):
    n, cap, width = laid.shape
    heads, tok, _ = q_heads.shape
    kv_count = kv_pack.shape[0]
    pairs = heads // 2
    hidden = gate_weight.shape[1]
    bf = jnp.bfloat16
    vmem = pl.BlockSpec(memory_space=pltpu.VMEM)
    anywhere = pl.BlockSpec(memory_space=pl.ANY)
    dma = pltpu.SemaphoreType.DMA
    return pl.pallas_call(
        functools.partial(fused_kernel, n),
        out_shape=(
            jax.ShapeDtypeStruct((n, cap, width), bf),
            jax.ShapeDtypeStruct((tok // 4, width), bf),
        ),
        in_specs=[vmem] * 3 + [anywhere] * 4,
        out_specs=(vmem, vmem),
        scratch_shapes=[
            pltpu.VMEM((width, hidden), bf),
            pltpu.VMEM((width, hidden), bf),
            pltpu.VMEM((hidden, width), bf),
            pltpu.VMEM((pairs, 128, width), bf),
            pltpu.VMEM((n, 4, cap, width), bf),
            pltpu.VMEM((n, 2, 2, cap, width), bf),
            pltpu.VMEM((n, 2, cap, width), bf),
            pltpu.VMEM((n, cap, width), bf),
            pltpu.VMEM((n, cap, width), bf),
            pltpu.VMEM((n, cap, width), bf),
            pltpu.VMEM((kv_count, n, tok, 128), bf),
            pltpu.VMEM((pairs, tok, 128), bf),
            pltpu.VMEM((2, 2, tok // 4, width), bf),
            pltpu.VMEM((2, tok // 4, width), bf),
            pltpu.VMEM((tok // 4, width), bf),
            pltpu.VMEM((tok // 4, width), bf),
            dma((6,)),
            dma((2, n)),
            dma((2, n)),
            dma((2, 3, n)),
            dma((2, 2, n)),
            dma((2, n)),
            dma((2, 2)),
        ],
        compiler_params=pltpu.CompilerParams(
            collective_id=0, has_side_effects=True, vmem_limit_bytes=62 * 1024 * 1024
        ),
    )(laid, q_heads, kv_pack, gate_weight, up_weight, down_weight, out_weight.reshape(pairs, 128, width))


def plain_shards(
    queries,
    keys,
    values,
    query_gain,
    key_gain,
    out_weight,
    expert_input,
    norm_gain,
    routes,
    route_weight,
    gate_weight,
    up_weight,
    down_weight,
):
    tok_mix = queries.shape[0]
    head_count = query_gain.shape[0] // HEAD_DIM
    kv_count = key_gain.shape[0] // HEAD_DIM
    group_size = head_count // kv_count
    offset = lax.axis_index("ep") * tok_mix
    q_turned = head_norm(queries, query_gain, head_count, offset)
    k_turned = head_norm(keys, key_gain, kv_count, offset)
    grouped = q_turned.reshape(tok_mix, kv_count, group_size, HEAD_DIM)
    score_scale = HEAD_DIM ** (-0.5)
    start_state = (
        jnp.full((kv_count, group_size, tok_mix), -jnp.inf, jnp.float32),
        jnp.zeros((kv_count, group_size, tok_mix), jnp.float32),
        jnp.zeros((tok_mix, kv_count, group_size, HEAD_DIM), jnp.float32),
    )
    running = start_state
    key_piece = lax.all_gather(k_turned, "ep", axis=0, tiled=True)
    value_piece = lax.all_gather(values, "ep", axis=0, tiled=True)
    length = key_piece.shape[0]
    block_len = length
    while block_len > 2048 and block_len % 2 == 0:
        block_len = block_len // 2
    key_blocks = key_piece.reshape(length // block_len, block_len, key_piece.shape[1])
    value_blocks = value_piece.reshape(length // block_len, block_len, value_piece.shape[1])

    def advance(inner_state, key_value):
        return (absorb(inner_state, key_value[0], key_value[1], grouped, score_scale), None)

    running, unused = lax.scan(advance, running, (key_blocks, value_blocks))
    final_max, weight_sum, summed = running
    attended = (
        (summed / jnp.transpose(weight_sum, (2, 0, 1))[..., None])
        .reshape(tok_mix, -1)
        .astype(jnp.bfloat16)
    )
    mixed = lax.psum_scatter(
        jnp.dot(attended, out_weight, preferred_element_type=jnp.float32).astype(jnp.bfloat16),
        "tp",
        scatter_dimension=0,
        tiled=True,
    )
    tok_exp = expert_input.shape[0]
    top_count = routes.shape[1]
    expert_count = lax.axis_size("ep")
    capacity = 2 * top_count * tok_exp // expert_count
    as_float = expert_input.astype(jnp.float32)
    normed = (
        as_float
        * lax.rsqrt(jnp.mean(as_float * as_float, axis=-1, keepdims=True) + NORM_EPS)
        * norm_gain
    ).astype(jnp.bfloat16)
    flat_routes = routes.reshape(-1)
    route_hits = (
        flat_routes[:, None] == jnp.arange(expert_count, dtype=jnp.int32)[None, :]
    ).astype(jnp.int32)
    slot_rank = jnp.sum((jnp.cumsum(route_hits, axis=0) - route_hits) * route_hits, axis=1)
    slot_ids = flat_routes * capacity + slot_rank
    placed = jnp.arange(expert_count * capacity, dtype=jnp.int32)[:, None] == slot_ids[None, :]
    placed = jnp.any(placed.reshape(expert_count * capacity, tok_exp, top_count), axis=2).astype(
        jnp.bfloat16
    )
    outbound = jnp.dot(placed, normed, preferred_element_type=jnp.float32).astype(jnp.bfloat16)
    model_width = outbound.shape[1]
    half_cap = capacity // 2
    laid = outbound.reshape(expert_count, capacity, model_width)
    first_half = run_experts(
        laid[:, :half_cap].reshape(expert_count * half_cap, model_width),
        gate_weight,
        up_weight,
        down_weight,
    )
    second_half = run_experts(
        laid[:, half_cap:].reshape(expert_count * half_cap, model_width),
        gate_weight,
        up_weight,
        down_weight,
    )
    back_rows = jnp.concatenate(
        [
            first_half.reshape(expert_count, half_cap, model_width),
            second_half.reshape(expert_count, half_cap, model_width),
        ],
        axis=1,
    )
    back_rows = back_rows.reshape(expert_count * capacity, model_width)
    picked = back_rows[slot_ids.reshape(tok_exp, top_count)]
    moe_out = jnp.sum(picked.astype(jnp.float32) * route_weight[:, :, None], axis=1).astype(
        jnp.bfloat16
    )
    return (mixed, moe_out)


def shards(
    queries,
    keys,
    values,
    query_gain,
    key_gain,
    out_weight,
    expert_input,
    norm_gain,
    routes,
    route_weight,
    gate_weight,
    up_weight,
    down_weight,
):
    tok_exp, model_width = expert_input.shape
    top_count = routes.shape[1]
    expert_count = lax.axis_size("ep")
    capacity = 2 * top_count * tok_exp // expert_count
    if capacity % 16 != 0 or lax.axis_size("tp") != 4:
        return plain_shards(
            queries,
            keys,
            values,
            query_gain,
            key_gain,
            out_weight,
            expert_input,
            norm_gain,
            routes,
            route_weight,
            gate_weight,
            up_weight,
            down_weight,
        )
    tok_mix = queries.shape[0]
    head_count = query_gain.shape[0] // HEAD_DIM
    kv_count = key_gain.shape[0] // HEAD_DIM
    offset = lax.axis_index("ep") * tok_mix
    q_turned = head_norm(queries, query_gain, head_count, offset)
    k_turned = head_norm(keys, key_gain, kv_count, offset)
    q_heads = jnp.transpose(q_turned.reshape(tok_mix, head_count, HEAD_DIM), (1, 0, 2))
    q_heads = jnp.pad(q_heads, ((0, 0), (0, 0), (0, HEAD_DIM)))
    kv_pack = jnp.concatenate(
        [k_turned.reshape(tok_mix, kv_count, HEAD_DIM), values.reshape(tok_mix, kv_count, HEAD_DIM)],
        axis=-1,
    )
    kv_pack = jnp.transpose(kv_pack, (1, 0, 2))
    as_float = expert_input.astype(jnp.float32)
    normed = (
        as_float
        * lax.rsqrt(jnp.mean(as_float * as_float, axis=-1, keepdims=True) + NORM_EPS)
        * norm_gain
    ).astype(jnp.bfloat16)
    flat_routes = routes.reshape(-1)
    route_hits = (
        flat_routes[:, None] == jnp.arange(expert_count, dtype=jnp.int32)[None, :]
    ).astype(jnp.int32)
    slot_rank = jnp.sum((jnp.cumsum(route_hits, axis=0) - route_hits) * route_hits, axis=1)
    slot_ids = (flat_routes * capacity + slot_rank).reshape(tok_exp, top_count)
    slots = jnp.arange(expert_count * capacity, dtype=jnp.int32)
    placed = jnp.any(slots[:, None, None] == slot_ids[None], axis=2).astype(jnp.bfloat16)
    outbound = jnp.dot(placed, normed, preferred_element_type=jnp.float32).astype(jnp.bfloat16)
    back_rows, mixed = fused(
        outbound.reshape(expert_count, capacity, model_width),
        q_heads,
        kv_pack,
        gate_weight[0],
        up_weight[0],
        down_weight[0],
        out_weight,
    )
    back_rows = back_rows.reshape(expert_count * capacity, model_width)
    moe_sum = jnp.zeros((tok_exp, model_width), jnp.float32)
    for k in range(top_count):
        chosen = (slot_ids[:, k, None] == slots[None, :]).astype(jnp.bfloat16)
        picked = jnp.dot(chosen, back_rows, preferred_element_type=jnp.float32)
        moe_sum = moe_sum + picked * route_weight[:, k, None]
    return (mixed, moe_sum.astype(jnp.bfloat16))


def solution(mesh):
    placed = (
        P("ep", "tp"),
        P("ep", "tp"),
        P("ep", "tp"),
        P("tp"),
        P("tp"),
        P("tp", None),
        P(("ep", "tp"), None),
        P(),
        P(("ep", "tp"), None),
        P(("ep", "tp"), None),
        P("ep", None, "tp"),
        P("ep", None, "tp"),
        P("ep", "tp", None),
    )
    return jax.shard_map(
        shards,
        mesh=mesh,
        in_specs=placed,
        out_specs=(P(("ep", "tp"), None), P(("ep", "tp"), None)),
        check_vma=False,
    )
```

```python
import functools

import jax
import jax.numpy as jnp
from jax import lax
from jax.experimental import pallas as pl
from jax.experimental.pallas import tpu as pltpu
from jax.sharding import PartitionSpec as P

HEAD_DIM = 64
GRID_W = 128


NORM_EPS = 1e-06
ROPE_BASE = 10000.0


def rotate(vectors, grid_rows, grid_cols):
    quarter = vectors.shape[-1] // 4
    inverse = ROPE_BASE ** (-jnp.arange(quarter, dtype=jnp.float32) / quarter)
    angle_row = grid_rows[:, None] * inverse
    angle_col = grid_cols[:, None] * inverse
    angles = jnp.concatenate([angle_row, angle_row, angle_col, angle_col], axis=-1)[:, None, :]
    part_one, part_two, part_three, part_four = jnp.split(vectors, 4, axis=-1)
    turned = jnp.concatenate([-part_two, part_one, -part_four, part_three], axis=-1)
    return vectors * jnp.cos(angles) + turned * jnp.sin(angles)


def head_norm(raw_rows, gains, head_count, offset):
    row_count = raw_rows.shape[0]
    flat_rows = raw_rows.astype(jnp.float32).reshape(row_count, head_count, -1)
    unit_vec = flat_rows * lax.rsqrt(
        jnp.mean(flat_rows * flat_rows, axis=-1, keepdims=True) + NORM_EPS
    )
    unit_vec = unit_vec * gains.reshape(head_count, -1)
    places = offset + jnp.arange(row_count, dtype=jnp.int32)
    grid_rows = (places // GRID_W).astype(jnp.float32)
    grid_cols = (places % GRID_W).astype(jnp.float32)
    return rotate(unit_vec, grid_rows, grid_cols).astype(jnp.bfloat16).reshape(row_count, -1)


def absorb(running, key_block, value_block, grouped, score_scale):
    run_max, weight_sum, summed = running
    kv_count = grouped.shape[1]
    key_heads = key_block.reshape(key_block.shape[0], kv_count, -1)
    value_heads = value_block.reshape(value_block.shape[0], kv_count, -1)
    scores = (
        jnp.einsum("qhgd,khd->hgqk", grouped, key_heads, preferred_element_type=jnp.float32)
        * score_scale
    )
    new_max = jnp.maximum(run_max, jnp.max(scores, axis=-1))
    rescale = jnp.exp(run_max - new_max)
    weights = jnp.exp(scores - new_max[..., None])
    weight_sum = weight_sum * rescale + jnp.sum(weights, axis=-1)
    update = jnp.einsum(
        "hgqk,khd->qhgd",
        weights.astype(jnp.bfloat16),
        value_heads,
        preferred_element_type=jnp.float32,
    )
    summed = summed * jnp.transpose(rescale, (2, 0, 1))[..., None] + update
    return (new_max, weight_sum, summed)


def run_experts(sending, gate_weight, up_weight, down_weight):
    arrived = lax.all_to_all(sending, "ep", split_axis=0, concat_axis=0, tiled=True)
    shard_rows = lax.all_gather(arrived, "tp", axis=0, tiled=True)
    gate_out = jnp.dot(shard_rows, gate_weight[0], preferred_element_type=jnp.float32)
    up_out = jnp.dot(shard_rows, up_weight[0], preferred_element_type=jnp.float32)
    hidden = (jax.nn.silu(gate_out) * up_out).astype(jnp.bfloat16)
    results = lax.psum_scatter(
        jnp.dot(hidden, down_weight[0], preferred_element_type=jnp.float32).astype(jnp.bfloat16),
        "tp",
        scatter_dimension=0,
        tiled=True,
    )
    return lax.all_to_all(results, "ep", split_axis=0, concat_axis=0, tiled=True)


MESH = pl.DeviceIdType.MESH
TILE = 1024


def flip(index, pattern, size):
    result = 0
    bit = 1
    while bit < size:
        both = lax.rem(lax.div(index, bit) + lax.div(pattern, bit), 2)
        result = result + both * bit
        bit = bit * 2
    return result


def fused_kernel(
    n,
    laid,
    q_ref,
    kv_ref,
    wg_hbm,
    wu_hbm,
    wd_hbm,
    ow_hbm,
    back,
    mixed,
    wg,
    wu,
    wd,
    ow,
    rows,
    partial,
    red,
    q_send,
    x_got,
    y_send,
    kv_all,
    attended,
    m_part,
    m_red,
    m_send,
    m_got,
    load_sem,
    kv_sems,
    disp_sems,
    fwd_sems,
    red_sems,
    ret_sems,
    mix_sems,
):
    e = lax.axis_index("ep")
    t = lax.axis_index("tp")
    side = lax.div(t, 2)
    core = lax.rem(t, 2)
    other_side = 1 - side
    other_core = 1 - core
    x_peer = (e, other_side * 2 + core)
    c_peer = (e, side * 2 + other_core)
    cap, width = laid.shape[1], laid.shape[2]
    pairs = attended.shape[0]
    tok = attended.shape[1]

    def remote(src, dst, send, recv, device):
        return pltpu.make_async_remote_copy(
            src_ref=src, dst_ref=dst, send_sem=send, recv_sem=recv, device_id=device, device_id_type=MESH
        )

    loads = [
        pltpu.make_async_copy(a, b, load_sem.at[k])
        for k, (a, b) in enumerate([(ow_hbm, ow), (wg_hbm, wg), (wu_hbm, wu), (wd_hbm, wd)])
    ]
    for load in loads:
        load.start()

    barrier = pltpu.get_barrier_semaphore()
    for s in range(1, n):
        pl.semaphore_signal(barrier, inc=1, device_id=(flip(e, s, n), t), device_id_type=MESH)
    pl.semaphore_signal(barrier, inc=1, device_id=x_peer, device_id_type=MESH)
    pl.semaphore_signal(barrier, inc=1, device_id=c_peer, device_id_type=MESH)
    pl.semaphore_wait(barrier, n + 1)

    def kv_direct(s):
        return remote(kv_ref, kv_all.at[:, e], kv_sems.at[0, s], kv_sems.at[1, s], (flip(e, s, n), t))

    def kv_direct_in(s):
        return remote(kv_ref, kv_all.at[:, flip(e, s, n)], kv_sems.at[0, s], kv_sems.at[1, s], (flip(e, s, n), t))

    def kv_relay(s):
        owner = flip(e, s, n)
        return remote(kv_all.at[:, owner], kv_all.at[:, owner], kv_sems.at[0, s + 1], kv_sems.at[1, s + 1], (flip(e, 1, n), t))

    def kv_relay_in(s):
        owner = flip(e, s + 1, n)
        return remote(kv_all.at[:, owner], kv_all.at[:, owner], kv_sems.at[0, s + 1], kv_sems.at[1, s + 1], (flip(e, 1, n), t))

    order = [0, 1] + sorted(range(2, n), key=lambda s: (s < 4, s % 2, -s))

    def pattern(i):
        chosen = order[0]
        for place in range(1, n):
            chosen = jnp.where(i == place, order[place], chosen)
        return chosen

    def dispatch(i):
        s = pattern(i)
        return remote(laid.at[flip(e, s, n)], rows.at[e, t], disp_sems.at[0, i], disp_sems.at[1, i], (flip(e, s, n), t))

    def dispatch_in(i):
        s = pattern(i)
        return remote(laid.at[flip(e, s, n)], rows.at[flip(e, s, n), t], disp_sems.at[0, i], disp_sems.at[1, i], (flip(e, s, n), t))

    def owner_of(i):
        return flip(e, pattern(i), n)

    def to_side(i):
        o = owner_of(i)
        return remote(rows.at[o, t], rows.at[o, t], fwd_sems.at[0, 0, i], fwd_sems.at[1, 0, i], x_peer)

    def from_side(i):
        o = owner_of(i)
        return remote(rows.at[o, t], rows.at[o, other_side * 2 + core], fwd_sems.at[0, 0, i], fwd_sems.at[1, 0, i], x_peer)

    def to_core(i):
        o = owner_of(i)
        return remote(rows.at[o, t], rows.at[o, t], fwd_sems.at[0, 1, i], fwd_sems.at[1, 1, i], c_peer)

    def from_core(i):
        o = owner_of(i)
        return remote(rows.at[o, t], rows.at[o, side * 2 + other_core], fwd_sems.at[0, 1, i], fwd_sems.at[1, 1, i], c_peer)

    def relay_core(i):
        o = owner_of(i)
        slot = other_side * 2 + core
        return remote(rows.at[o, slot], rows.at[o, slot], fwd_sems.at[0, 2, i], fwd_sems.at[1, 2, i], c_peer)

    def relayed_core(i):
        o = owner_of(i)
        slot = other_side * 2 + core
        return remote(rows.at[o, slot], rows.at[o, other_side * 2 + other_core], fwd_sems.at[0, 2, i], fwd_sems.at[1, 2, i], c_peer)

    def reduce_core(i):
        return remote(partial.at[i, :, other_core], red.at[i], red_sems.at[0, 0, i], red_sems.at[1, 0, i], c_peer)

    def reduce_side(i):
        return remote(q_send.at[i], x_got.at[i], red_sems.at[0, 1, i], red_sems.at[1, 1, i], x_peer)

    def give_back(i):
        o = owner_of(i)
        return remote(y_send.at[i], back.at[e], ret_sems.at[0, i], ret_sems.at[1, i], (o, t))

    def get_back(i):
        o = owner_of(i)
        return remote(y_send.at[i], back.at[o], ret_sems.at[0, i], ret_sems.at[1, i], (o, t))

    mix_core = remote(m_part.at[:, other_core], m_red, mix_sems.at[0, 0], mix_sems.at[1, 0], c_peer)
    mix_side = remote(m_send, m_got, mix_sems.at[0, 1], mix_sems.at[1, 1], x_peer)

    own = pltpu.make_async_copy(laid.at[e], rows.at[e, t], load_sem.at[4])
    own_kv = pltpu.make_async_copy(kv_ref, kv_all.at[:, e], load_sem.at[5])
    own.start()
    own_kv.start()
    for i in range(1, n):
        if i == 8:
            for s in range(2, n, 2):
                kv_direct(s).start()
            kv_direct(1).start()
        dispatch(i).start()
    for s in range(2, n, 2):
        kv_direct(s).start()
    kv_direct(1).start()
    own.wait()
    to_side(0).start()
    to_core(0).start()
    own_kv.wait()

    def attend(pair):
        kv = kv_all[lax.div(pair * 2 * kv_all.shape[0], pairs * 2)].reshape(n * tok, 128)
        halves = []
        for h in range(2):
            scores = lax.dot_general(
                q_ref[pair * 2 + h], kv, (((1,), (1,)), ((), ())), preferred_element_type=jnp.float32
            ) * (HEAD_DIM ** (-0.5))
            peak = jnp.max(scores, axis=1, keepdims=True)
            weights = jnp.exp(scores - peak)
            total = jnp.sum(weights, axis=1, keepdims=True)
            summed = jnp.dot(weights.astype(jnp.bfloat16), kv, preferred_element_type=jnp.float32)
            halves.append(summed / total)
        lane = lax.broadcasted_iota(jnp.int32, halves[0].shape, 1)
        joined = jnp.where(lane < HEAD_DIM, pltpu.roll(halves[0], HEAD_DIM, 1), halves[1])
        attended[pair] = joined.astype(jnp.bfloat16)

    def f32(value):
        return value.astype(jnp.float32)

    def step(i, carry):
        @pl.when(jnp.logical_and(i > 0, i < n))
        def _():
            dispatch_in(i).wait_recv()
            to_side(i).start()
            to_core(i).start()

        @pl.when(i == 6)
        def _():
            for s in range(2, n, 2):
                kv_direct_in(s).wait_recv()
                kv_relay(s).start()

        @pl.when(jnp.logical_and(i >= 1, i <= n))
        def _():
            from_side(i - 1).wait_recv()
            relay_core(i - 1).start()

        @pl.when(i == 7)
        def _():
            kv_direct_in(1).wait_recv()
            for s in range(2, n, 2):
                kv_relay_in(s).wait_recv()

        @pl.when(jnp.logical_and(i >= 7, i < 7 + pairs // 2))
        def _():
            attend(2 * (i - 7))
            attend(2 * (i - 7) + 1)

        @pl.when(i == 7 + pairs // 2)
        def _():
            loads[0].wait()
            for tile in range(0, width, TILE):
                product = jnp.dot(attended[0], ow[0, :, tile:tile + TILE], preferred_element_type=jnp.float32)
                for p in range(1, pairs):
                    product += jnp.dot(attended[p], ow[p, :, tile:tile + TILE], preferred_element_type=jnp.float32)
                m_part[:, :, :, tile:tile + TILE] = product.astype(jnp.bfloat16).reshape(2, 2, tok // 4, TILE)
            mix_core.start()

        @pl.when(jnp.logical_and(i >= 1, i <= n))
        def _():
            k = i - 1

            @pl.when(k == 0)
            def _():
                for load in loads[1:]:
                    load.wait()

            from_core(k).wait_recv()
            relayed_core(k).wait_recv()
            tokens = rows[owner_of(k)].reshape(4 * cap, width)
            gate = jnp.dot(tokens, wg[...], preferred_element_type=jnp.float32)
            up = jnp.dot(tokens, wu[...], preferred_element_type=jnp.float32)
            hidden = (gate / (1.0 + jnp.exp(-gate)) * up).astype(jnp.bfloat16)
            for tile in range(0, width, TILE):
                product = jnp.dot(hidden, wd[:, tile:tile + TILE], preferred_element_type=jnp.float32)
                partial[k, :, :, :, tile:tile + TILE] = product.astype(jnp.bfloat16).reshape(2, 2, cap, TILE)
            reduce_core(k).start()

        @pl.when(i == 7 + pairs // 2)
        def _():
            mix_core.wait_recv()
            m_send[...] = (f32(m_part[other_side, core]) + f32(m_red[other_side])).astype(jnp.bfloat16)
            mix_side.start()

        @pl.when(jnp.logical_and(i >= 2, i < n + 2))
        def _():
            k = i - 2
            reduce_side(k).wait_recv()
            y = (f32(partial[k, side, core]) + f32(red[k, side]) + f32(x_got[k])).astype(jnp.bfloat16)

            @pl.when(k == 0)
            def _():
                back[e] = y

            @pl.when(k > 0)
            def _():
                y_send[k] = y
                give_back(k).start()

        @pl.when(jnp.logical_and(i >= 1, i <= n))
        def _():
            k = i - 1
            reduce_core(k).wait_recv()
            q_send[k] = (f32(partial[k, other_side, core]) + f32(red[k, other_side])).astype(jnp.bfloat16)
            reduce_side(k).start()

        return carry

    lax.fori_loop(0, n + 2, step, 0)

    mix_side.wait_recv()
    mixed[...] = (f32(m_part[side, core]) + f32(m_red[side]) + f32(m_got[...])).astype(jnp.bfloat16)
    mix_core.wait_send()
    mix_side.wait_send()
    for s in range(2, n, 2):
        kv_direct(s).wait_send()
        kv_relay(s).wait_send()
    kv_direct(1).wait_send()

    def drain(i, carry):
        @pl.when(i > 0)
        def _():
            dispatch(i).wait_send()
            give_back(i).wait_send()
            get_back(i).wait_recv()

        to_side(i).wait_send()
        to_core(i).wait_send()
        relay_core(i).wait_send()
        reduce_core(i).wait_send()
        reduce_side(i).wait_send()
        return carry

    lax.fori_loop(0, n, drain, 0)


def fused(laid, q_heads, kv_pack, gate_weight, up_weight, down_weight, out_weight):
    n, cap, width = laid.shape
    heads, tok, _ = q_heads.shape
    kv_count = kv_pack.shape[0]
    pairs = heads // 2
    hidden = gate_weight.shape[1]
    bf = jnp.bfloat16
    vmem = pl.BlockSpec(memory_space=pltpu.VMEM)
    anywhere = pl.BlockSpec(memory_space=pl.ANY)
    dma = pltpu.SemaphoreType.DMA
    return pl.pallas_call(
        functools.partial(fused_kernel, n),
        out_shape=(
            jax.ShapeDtypeStruct((n, cap, width), bf),
            jax.ShapeDtypeStruct((tok // 4, width), bf),
        ),
        in_specs=[vmem] * 3 + [anywhere] * 4,
        out_specs=(vmem, vmem),
        scratch_shapes=[
            pltpu.VMEM((width, hidden), bf),
            pltpu.VMEM((width, hidden), bf),
            pltpu.VMEM((hidden, width), bf),
            pltpu.VMEM((pairs, 128, width), bf),
            pltpu.VMEM((n, 4, cap, width), bf),
            pltpu.VMEM((n, 2, 2, cap, width), bf),
            pltpu.VMEM((n, 2, cap, width), bf),
            pltpu.VMEM((n, cap, width), bf),
            pltpu.VMEM((n, cap, width), bf),
            pltpu.VMEM((n, cap, width), bf),
            pltpu.VMEM((kv_count, n, tok, 128), bf),
            pltpu.VMEM((pairs, tok, 128), bf),
            pltpu.VMEM((2, 2, tok // 4, width), bf),
            pltpu.VMEM((2, tok // 4, width), bf),
            pltpu.VMEM((tok // 4, width), bf),
            pltpu.VMEM((tok // 4, width), bf),
            dma((6,)),
            dma((2, n)),
            dma((2, n)),
            dma((2, 3, n)),
            dma((2, 2, n)),
            dma((2, n)),
            dma((2, 2)),
        ],
        compiler_params=pltpu.CompilerParams(
            collective_id=0, has_side_effects=True, vmem_limit_bytes=62 * 1024 * 1024
        ),
    )(laid, q_heads, kv_pack, gate_weight, up_weight, down_weight, out_weight.reshape(pairs, 128, width))


def plain_shards(
    queries,
    keys,
    values,
    query_gain,
    key_gain,
    out_weight,
    expert_input,
    norm_gain,
    routes,
    route_weight,
    gate_weight,
    up_weight,
    down_weight,
):
    tok_mix = queries.shape[0]
    head_count = query_gain.shape[0] // HEAD_DIM
    kv_count = key_gain.shape[0] // HEAD_DIM
    group_size = head_count // kv_count
    offset = lax.axis_index("ep") * tok_mix
    q_turned = head_norm(queries, query_gain, head_count, offset)
    k_turned = head_norm(keys, key_gain, kv_count, offset)
    grouped = q_turned.reshape(tok_mix, kv_count, group_size, HEAD_DIM)
    score_scale = HEAD_DIM ** (-0.5)
    start_state = (
        jnp.full((kv_count, group_size, tok_mix), -jnp.inf, jnp.float32),
        jnp.zeros((kv_count, group_size, tok_mix), jnp.float32),
        jnp.zeros((tok_mix, kv_count, group_size, HEAD_DIM), jnp.float32),
    )
    running = start_state
    key_piece = lax.all_gather(k_turned, "ep", axis=0, tiled=True)
    value_piece = lax.all_gather(values, "ep", axis=0, tiled=True)
    length = key_piece.shape[0]
    block_len = length
    while block_len > 2048 and block_len % 2 == 0:
        block_len = block_len // 2
    key_blocks = key_piece.reshape(length // block_len, block_len, key_piece.shape[1])
    value_blocks = value_piece.reshape(length // block_len, block_len, value_piece.shape[1])

    def advance(inner_state, key_value):
        return (absorb(inner_state, key_value[0], key_value[1], grouped, score_scale), None)

    running, unused = lax.scan(advance, running, (key_blocks, value_blocks))
    final_max, weight_sum, summed = running
    attended = (
        (summed / jnp.transpose(weight_sum, (2, 0, 1))[..., None])
        .reshape(tok_mix, -1)
        .astype(jnp.bfloat16)
    )
    mixed = lax.psum_scatter(
        jnp.dot(attended, out_weight, preferred_element_type=jnp.float32).astype(jnp.bfloat16),
        "tp",
        scatter_dimension=0,
        tiled=True,
    )
    tok_exp = expert_input.shape[0]
    top_count = routes.shape[1]
    expert_count = lax.axis_size("ep")
    capacity = 2 * top_count * tok_exp // expert_count
    as_float = expert_input.astype(jnp.float32)
    normed = (
        as_float
        * lax.rsqrt(jnp.mean(as_float * as_float, axis=-1, keepdims=True) + NORM_EPS)
        * norm_gain
    ).astype(jnp.bfloat16)
    flat_routes = routes.reshape(-1)
    route_hits = (
        flat_routes[:, None] == jnp.arange(expert_count, dtype=jnp.int32)[None, :]
    ).astype(jnp.int32)
    slot_rank = jnp.sum((jnp.cumsum(route_hits, axis=0) - route_hits) * route_hits, axis=1)
    slot_ids = flat_routes * capacity + slot_rank
    placed = jnp.arange(expert_count * capacity, dtype=jnp.int32)[:, None] == slot_ids[None, :]
    placed = jnp.any(placed.reshape(expert_count * capacity, tok_exp, top_count), axis=2).astype(
        jnp.bfloat16
    )
    outbound = jnp.dot(placed, normed, preferred_element_type=jnp.float32).astype(jnp.bfloat16)
    model_width = outbound.shape[1]
    half_cap = capacity // 2
    laid = outbound.reshape(expert_count, capacity, model_width)
    first_half = run_experts(
        laid[:, :half_cap].reshape(expert_count * half_cap, model_width),
        gate_weight,
        up_weight,
        down_weight,
    )
    second_half = run_experts(
        laid[:, half_cap:].reshape(expert_count * half_cap, model_width),
        gate_weight,
        up_weight,
        down_weight,
    )
    back_rows = jnp.concatenate(
        [
            first_half.reshape(expert_count, half_cap, model_width),
            second_half.reshape(expert_count, half_cap, model_width),
        ],
        axis=1,
    )
    back_rows = back_rows.reshape(expert_count * capacity, model_width)
    picked = back_rows[slot_ids.reshape(tok_exp, top_count)]
    moe_out = jnp.sum(picked.astype(jnp.float32) * route_weight[:, :, None], axis=1).astype(
        jnp.bfloat16
    )
    return (mixed, moe_out)


def shards(
    queries,
    keys,
    values,
    query_gain,
    key_gain,
    out_weight,
    expert_input,
    norm_gain,
    routes,
    route_weight,
    gate_weight,
    up_weight,
    down_weight,
):
    tok_exp, model_width = expert_input.shape
    top_count = routes.shape[1]
    expert_count = lax.axis_size("ep")
    capacity = 2 * top_count * tok_exp // expert_count
    if capacity % 16 != 0 or lax.axis_size("tp") != 4:
        return plain_shards(
            queries,
            keys,
            values,
            query_gain,
            key_gain,
            out_weight,
            expert_input,
            norm_gain,
            routes,
            route_weight,
            gate_weight,
            up_weight,
            down_weight,
        )
    tok_mix = queries.shape[0]
    head_count = query_gain.shape[0] // HEAD_DIM
    kv_count = key_gain.shape[0] // HEAD_DIM
    offset = lax.axis_index("ep") * tok_mix
    q_turned = head_norm(queries, query_gain, head_count, offset)
    k_turned = head_norm(keys, key_gain, kv_count, offset)
    q_heads = jnp.transpose(q_turned.reshape(tok_mix, head_count, HEAD_DIM), (1, 0, 2))
    q_heads = jnp.pad(q_heads, ((0, 0), (0, 0), (0, HEAD_DIM)))
    kv_pack = jnp.concatenate(
        [k_turned.reshape(tok_mix, kv_count, HEAD_DIM), values.reshape(tok_mix, kv_count, HEAD_DIM)],
        axis=-1,
    )
    kv_pack = jnp.transpose(kv_pack, (1, 0, 2))
    as_float = expert_input.astype(jnp.float32)
    normed = (
        as_float
        * lax.rsqrt(jnp.mean(as_float * as_float, axis=-1, keepdims=True) + NORM_EPS)
        * norm_gain
    ).astype(jnp.bfloat16)
    flat_routes = routes.reshape(-1)
    route_hits = (
        flat_routes[:, None] == jnp.arange(expert_count, dtype=jnp.int32)[None, :]
    ).astype(jnp.int32)
    slot_rank = jnp.sum((jnp.cumsum(route_hits, axis=0) - route_hits) * route_hits, axis=1)
    slot_ids = (flat_routes * capacity + slot_rank).reshape(tok_exp, top_count)
    slots = jnp.arange(expert_count * capacity, dtype=jnp.int32)
    placed = jnp.any(slots[:, None, None] == slot_ids[None], axis=2).astype(jnp.bfloat16)
    outbound = jnp.dot(placed, normed, preferred_element_type=jnp.float32).astype(jnp.bfloat16)
    back_rows, mixed = fused(
        outbound.reshape(expert_count, capacity, model_width),
        q_heads,
        kv_pack,
        gate_weight[0],
        up_weight[0],
        down_weight[0],
        out_weight,
    )
    back_rows = back_rows.reshape(expert_count * capacity, model_width)
    moe_sum = jnp.zeros((tok_exp, model_width), jnp.float32)
    for k in range(top_count):
        chosen = (slot_ids[:, k, None] == slots[None, :]).astype(jnp.bfloat16)
        picked = jnp.dot(chosen, back_rows, preferred_element_type=jnp.float32)
        moe_sum = moe_sum + picked * route_weight[:, k, None]
    return (mixed, moe_sum.astype(jnp.bfloat16))


def solution(mesh):
    placed = (
        P("ep", "tp"),
        P("ep", "tp"),
        P("ep", "tp"),
        P("tp"),
        P("tp"),
        P("tp", None),
        P(("ep", "tp"), None),
        P(),
        P(("ep", "tp"), None),
        P(("ep", "tp"), None),
        P("ep", None, "tp"),
        P("ep", None, "tp"),
        P("ep", "tp", None),
    )
    return jax.shard_map(
        shards,
        mesh=mesh,
        in_specs=placed,
        out_specs=(P(("ep", "tp"), None), P(("ep", "tp"), None)),
        check_vma=False,
    )
```
